32 devices in a mesh: sp: 8 (over z, y), tp: 4 (over x, core).
Axes of the slice: x: 2, y: 2, z: 4, core: 2. Of those that a mesh axis runs over, the one named last changes fastest.
Arguments:
- target: bfloat16 [1024, 2048], P('sp'), may hold values from -160 to 160
- source: bfloat16 [2048, 2048], P(('sp', 'tp')), may hold values from -160 to 160
- query_gain: float32 [2048], replicated, may hold values from 0.1 to 1.9
- source_gain: float32 [2048], replicated, may hold values from 0.1 to 1.9
- query_weight: bfloat16 [2048, 2048], P(None, 'tp'), may hold values from -4 to 4
- key_weight: bfloat16 [2048, 512], replicated, may hold values from -4 to 4
- value_weight: bfloat16 [2048, 512], replicated, may hold values from -1 to 1
- out_weight: bfloat16 [2048, 2048], P('tp'), may hold values from -0.125 to 0.125
- mixer_gain: float32 [2048], replicated, may hold values from 0.1 to 1.9
- gate_weight: bfloat16 [2048, 3072], P(None, 'tp'), may hold values from -0.125 to 0.125
- up_weight: bfloat16 [2048, 3072], P(None, 'tp'), may hold values from -0.125 to 0.125
- gate_taps: bfloat16 [3, 3072], P(None, 'tp'), may hold values from -3.5 to 3.5
- up_taps: bfloat16 [3, 3072], P(None, 'tp'), may hold values from -3.5 to 3.5
- down_weight: bfloat16 [3072, 2048], P('tp'), may hold values from -0.109375 to 0.109375
- final_gain: float32 [2048], replicated, may hold values from 0.1 to 1.9
Outputs:
- layer_out: bfloat16 [1024, 2048], P(('sp', 'tp'))
The draws below stay inside these ranges and needn't reach their ends.
All inputs are finite; a program needn't handle non-finite values.
Results may differ from the reference program's by a relative error of at most 0.012.
Values may be sent and summed in bfloat16 or wider, within the bound.
A program may use at most 64 MiB of HBM per device.

```python
import math
import jax
import jax.numpy as jnp
from jax import lax

D = 2048
HEADS = 8
HEAD = 256
KV_HEADS = 2
FF = 3072
CONV = 3
TGT_DEV = 128
SRC_DEV = 256
TGT = 1024
SRC = 2048
N_SP = 8
N_TP = 4


def draw_target(key, part):
    result = jax.random.truncated_normal(jax.random.fold_in(key, 11), -4.0, 4.0, (TGT, D), jnp.float32)
    return result.astype(jnp.bfloat16)


def draw_source(key, part):
    result = jax.random.truncated_normal(jax.random.fold_in(key, 31), -4.0, 4.0, (SRC, D), jnp.float32)
    return result.astype(jnp.bfloat16)


def drawn_weight(key, salt, columns):
    drawn = jax.random.truncated_normal(jax.random.fold_in(key, salt), -4.0, 4.0, (D, columns), jnp.float32)
    drawn = drawn * math.sqrt(2.5 / D)
    return drawn.astype(jnp.bfloat16)


def draw_query_weight(key, part):
    return drawn_weight(key, 21, HEADS * HEAD)


def draw_key_weight(key, part):
    return drawn_weight(key, 22, KV_HEADS * HEAD)


def block_scale(own_key, dims, shards, low, top_value):
    level, own = 1.0, jax.random.fold_in(own_key, 6)
    for axis_at, blocks in shards:
        heights = jnp.exp(jax.random.uniform(jax.random.fold_in(own, axis_at), (blocks,), jnp.float32, low / len(shards), top_value / len(shards)))
        level = level * jnp.repeat(heights, dims[axis_at] // blocks).reshape([-1 if axis == axis_at else 1 for axis in range(len(dims))])
    return level


def noise(key, dims, spread, reach, split=(), dtype=jnp.bfloat16):
    entries = spread * jax.random.normal(key, dims, jnp.float32)
    if split:
        entries = entries * block_scale(key, dims, split, -0.22, 0.18)
    return jnp.clip(entries, -reach, reach).astype(dtype)


def setup_inputs(seed: int = 0) -> dict:
    key_of = jax.random.split(jax.random.key(seed), 16)
    target = draw_target(jax.random.fold_in(key_of[15], 71), 0)
    source = draw_source(jax.random.fold_in(key_of[15], 71), 0)
    query_gain = jnp.clip(1.0 + 0.18 * jax.random.normal(key_of[2], (D,), jnp.float32), 0.1, 1.9)
    source_gain = jnp.clip(1.0 + 0.18 * jax.random.normal(key_of[3], (D,), jnp.float32), 0.1, 1.9)
    query_weight = draw_query_weight(jax.random.fold_in(key_of[15], 71), 0)
    key_weight = draw_key_weight(jax.random.fold_in(key_of[15], 71), 0)
    value_weight = noise(key_of[6], (D, KV_HEADS * HEAD), (D // 48) ** -0.5, 1.0)
    out_weight = noise(key_of[7], (HEADS * HEAD, D), (HEADS * HEAD) ** -0.5, 0.125, ((0, 4),))
    mixer_gain = jnp.clip(1.0 + 0.18 * jax.random.normal(key_of[8], (D,), jnp.float32), 0.1, 1.9)
    gate_weight = noise(key_of[9], (D, FF), D ** -0.5, 0.125, ((1, 4),))
    up_weight = noise(key_of[10], (D, FF), D ** -0.5, 0.125, ((1, 4),))
    gate_taps = noise(key_of[11], (CONV, FF), CONV ** -0.5, 3.5, ((1, 4),))
    up_taps = noise(key_of[12], (CONV, FF), CONV ** -0.5, 3.5, ((1, 4),))
    down_weight = noise(key_of[13], (FF, D), FF ** -0.5, 0.109375, ((0, 4),))
    final_gain = jnp.clip(1.0 + 0.18 * jax.random.normal(key_of[14], (D,), jnp.float32), 0.1, 1.9)
    return {"target": target, "source": source, "query_gain": query_gain, "source_gain": source_gain, "query_weight": query_weight, "key_weight": key_weight, "value_weight": value_weight, "out_weight": out_weight, "mixer_gain": mixer_gain, "gate_weight": gate_weight, "up_weight": up_weight, "gate_taps": gate_taps, "up_taps": up_taps, "down_weight": down_weight, "final_gain": final_gain}


EPS = 1e-06

def normalize(values, gain):
    widened = values.astype(jnp.float32)
    scaled = widened * lax.rsqrt(lax.optimization_barrier(jnp.mean(widened * widened, axis=-1, keepdims=True)) + EPS)
    return (scaled * gain.astype(jnp.float32)).astype(jnp.bfloat16)

def rounded(values):
    return lax.optimization_barrier(values.astype(jnp.bfloat16)).astype(jnp.float32)

def reference(target, source, query_gain, source_gain, query_weight, key_weight, value_weight, out_weight, mixer_gain, gate_weight, up_weight, gate_taps, up_taps, down_weight, final_gain):
    group_size = HEADS // KV_HEADS
    slice_rows = SRC_DEV // N_TP
    normed = normalize(target, query_gain)
    queries = rounded(jnp.dot(normed, query_weight, preferred_element_type=jnp.float32))
    source_normed = normalize(source, source_gain)
    key_rows = rounded(jnp.dot(source_normed, key_weight, preferred_element_type=jnp.float32))
    value_rows = rounded(jnp.dot(source_normed, value_weight, preferred_element_type=jnp.float32))
    key_slices = key_rows.reshape(N_SP, N_TP, slice_rows, KV_HEADS, HEAD)
    value_slices = value_rows.reshape(N_SP, N_TP, slice_rows, KV_HEADS, HEAD)
    query_blocks = queries.reshape(N_SP, TGT_DEV, KV_HEADS, group_size, HEAD)
    score_scale = HEAD ** (-0.5)

    def attend(query_block):
        maxima = []
        sums = []
        partial_sums = []
        for slot in range(N_TP):
            slot_keys = key_slices[:, slot].reshape(N_SP * slice_rows, KV_HEADS, HEAD)
            slot_values = value_slices[:, slot].reshape(N_SP * slice_rows, KV_HEADS, HEAD)
            scores = jnp.einsum('bgjd,ngd->gjbn', query_block, slot_keys) * score_scale
            highest = lax.optimization_barrier(jnp.max(scores, axis=-1))
            weights = jnp.exp(scores - highest[..., None])
            maxima.append(highest)
            sums.append(lax.optimization_barrier(jnp.sum(weights, axis=-1)))
            partial_sums.append(jnp.einsum('gjbn,ngd->gjbd', rounded(weights), slot_values))
        maxima = jnp.stack(maxima)
        sums = jnp.stack(sums)
        partial_sums = jnp.stack(partial_sums)
        overall = lax.optimization_barrier(jnp.max(maxima, axis=0))
        factor = jnp.exp(maxima - overall)
        denominator = lax.optimization_barrier(jnp.sum(factor * sums, axis=0))
        merged = lax.optimization_barrier(jnp.sum(factor[..., None] * partial_sums, axis=0)) / denominator[..., None]
        return merged.transpose(2, 0, 1, 3).reshape(TGT_DEV, HEADS * HEAD).astype(jnp.bfloat16)
    attended = lax.map(attend, query_blocks).reshape(N_SP * TGT_DEV, HEADS * HEAD)
    projected = jnp.dot(attended, out_weight, preferred_element_type=jnp.float32)
    residual = (target.astype(jnp.float32) + projected).astype(jnp.bfloat16)
    mixer_in = normalize(residual, mixer_gain)
    gate_rows = rounded(jnp.dot(mixer_in, gate_weight, preferred_element_type=jnp.float32))
    up_rows = rounded(jnp.dot(mixer_in, up_weight, preferred_element_type=jnp.float32))
    stacked = jnp.stack([gate_rows, up_rows])
    padded = jnp.pad(stacked, ((0, 0), (CONV - 1, 0), (0, 0)))
    conv_taps = jnp.stack([gate_taps, up_taps]).astype(jnp.float32)
    total_rows = N_SP * TGT_DEV
    mixed = conv_taps[:, 0:1, :] * padded[:, 0:total_rows, :]
    for index_tap in range(1, CONV):
        mixed = mixed + conv_taps[:, index_tap:index_tap + 1, :] * padded[:, index_tap:index_tap + total_rows, :]
    hidden = (jax.nn.silu(mixed[0]) * mixed[1]).astype(jnp.bfloat16)
    mixer = jnp.dot(hidden, down_weight, preferred_element_type=jnp.float32)
    return normalize(residual.astype(jnp.float32) + mixer, final_gain)
```

```python
import functools

import jax
import jax.numpy as jnp
from jax import lax
from jax.experimental import pallas as pl
from jax.experimental.pallas import tpu as pltpu
from jax.sharding import PartitionSpec as P

MESH = pl.DeviceIdType.MESH
EPS = 1e-06
HALO = 16
CORES = 2
F32 = jnp.float32
BF16 = jnp.bfloat16


def normed(values, gain):
    wide = values.astype(F32)
    scale = lax.rsqrt(jnp.mean(wide * wide, axis=-1, keepdims=True) + EPS)
    return (wide * scale * gain).astype(BF16)


def layer(
    dims,
    target_h,
    source_h,
    qgain_h,
    sgain_h,
    qw_h,
    kw_h,
    vw_h,
    ow_h,
    mgain_h,
    gw_h,
    uw_h,
    gtaps_h,
    utaps_h,
    dw_h,
    fgain_h,
    out_ref,
    tgt,
    src,
    qgain,
    sgain,
    qw,
    kw,
    vw,
    ow,
    mgain,
    gw,
    uw,
    gtaps,
    utaps,
    dw,
    fgain,
    kvh,
    kv,
    q2,
    top,
    tot,
    acc,
    att,
    part,
    half_s,
    half_r,
    chip_s,
    chip_r,
    res,
    rows_in,
    conv_g,
    conv_u,
    hid,
    tail_s,
    tail_r,
    end_s,
    end_r,
    load_sem,
    kx_s,
    kx_r,
    cw_s,
    cw_r,
    cc_s,
    cc_r,
    d2_s,
    d2_r,
    b_s,
    b_r,
    bx_s,
    bx_r,
    m_s,
    m_r,
    h_s,
    h_r,
    f_s,
    f_r,
    fx_s,
    fx_r,
):
    n, chips, kv_heads, head, heads_here, cols = dims
    tgt_rows, width = tgt.shape
    r = src.shape[0]
    rs = tgt_rows // (CORES * chips)
    half_rows = chips * rs
    chunks = width // cols
    sp = lax.axis_index("sp")
    tp = lax.axis_index("tp")
    chip = tp // CORES
    core = tp % CORES
    mate = tp + 1 - 2 * core

    def chip_at(k):
        return (chip + k) % chips

    def ring_at(p):
        if n % 2:
            return p
        upper = p // (n // 2)
        return 2 * (p * (1 - upper) + (n - 1 - p) * upper) + upper

    if n % 2:
        pos = sp
    else:
        pos = (sp // 2) * (1 - sp % 2) + (n - 1 - sp // 2) * (sp % 2)
    ahead = ring_at((pos + 1) % n)
    behind = ring_at((pos + n - 1) % n)

    def load(index, hbm, vmem):
        copy = pltpu.make_async_copy(hbm, vmem, load_sem.at[index])
        copy.start()
        return copy

    first = [
        load(i, a, b)
        for i, (a, b) in enumerate(((source_h, src), (sgain_h, sgain), (kw_h, kw), (vw_h, vw)))
    ]
    second = [
        load(4 + i, a, b)
        for i, (a, b) in enumerate(((target_h, tgt), (qgain_h, qgain), (qw_h, qw)))
    ]

    barrier = pltpu.get_barrier_semaphore()
    following, previous = (sp + 1) % n, (sp + n - 1) % n
    peers = [(ahead, tp), (behind, tp), (sp, mate)]
    peers += [(sp, chip_at(k) * CORES + core) for k in range(1, chips)]
    peers += [(s, t) for s in (following, previous) for t in (tp, mate)]
    for peer in peers:
        pl.semaphore_signal(barrier, inc=1, device_id=peer, device_id_type=MESH)

    def remote(source_ref, dest_ref, send, recv, device):
        return pltpu.make_async_remote_copy(
            src_ref=source_ref,
            dst_ref=dest_ref,
            send_sem=send,
            recv_sem=recv,
            device_id=device,
            device_id_type=MESH,
        )

    def block(slot, lineage, j):
        start = ((slot * CORES + lineage) * chips + j) * r
        if not isinstance(start, int):
            start = pl.multiple_of(start, r)
        return kv.at[pl.ds(start, r), :]

    def head_of(c):
        return (c * CORES * kv_heads) // (chips * CORES)

    def chip_copy(k):
        there = chip_at(k)
        return remote(
            kvh.at[head_of(there)],
            block(0, 0, k),
            kx_s.at[k],
            kx_r.at[k],
            (sp, there * CORES + core),
        )

    last = n // 2 if n % 2 == 0 else 0
    full = (n - 1) // 2
    last_cw = (chips + 1) // 2

    def cw_slot(d):
        return 2 * d - 1

    def cc_slot(d):
        return n - 1 if isinstance(d, int) and d == last else 2 * d

    def cw_copy(d, j):
        held = 0 if isinstance(d, int) and d == 1 else cw_slot(d - 1)
        return remote(
            block(held, 0, j), block(cw_slot(d), 0, j), cw_s.at[d, j], cw_r.at[d, j], (ahead, tp)
        )

    def cc_copy(d, j):
        held = 0 if isinstance(d, int) and d == 1 else 2 * (d - 1)
        return remote(
            block(held, 0, j), block(cc_slot(d), 0, j), cc_s.at[d, j], cc_r.at[d, j], (behind, tp)
        )

    def mate_copy(slot, j):
        return remote(
            block(slot, 0, j), block(slot, 1, j), d2_s.at[slot, j], d2_r.at[slot, j], (sp, mate)
        )

    for copy in first:
        copy.wait()
    rest = [
        load(7 + i, a, b)
        for i, (a, b) in enumerate(
            (
                (ow_h, ow),
                (mgain_h, mgain),
                (gw_h, gw),
                (uw_h, uw),
                (gtaps_h, gtaps),
                (utaps_h, utaps),
                (dw_h, dw),
                (fgain_h, fgain),
            )
        )
    ]
    source_in = normed(src[...], sgain[...])
    keys = jnp.dot(source_in, kw[...], preferred_element_type=F32).astype(BF16)
    values = jnp.dot(source_in, vw[...], preferred_element_type=F32).astype(BF16)
    for g in range(kv_heads):
        kvh[g, :, :head] = keys[:, g * head : (g + 1) * head]
        kvh[g, :, head:] = values[:, g * head : (g + 1) * head]
    kv[0:r, :] = kvh[head_of(chip)]
    pl.semaphore_wait(barrier, len(peers))

    def launch(j):
        if n > 2 or j < last_cw:
            cw_copy(1, j).start()
        if n > 2 or j >= last_cw:
            cc_copy(1, j).start()
        mate_copy(0, j).start()

    for k in range(1, chips):
        chip_copy(k).start()
    launch(0)

    for copy in second:
        copy.wait()
    queries = jnp.dot(normed(tgt[...], qgain[...]), qw[...], preferred_element_type=F32).astype(
        BF16
    )
    for h in range(heads_here):
        q2[h * tgt_rows : (h + 1) * tgt_rows, :] = queries[:, h * head : (h + 1) * head]
    top[...] = jnp.full(top.shape, -1e30, F32)
    tot[...] = jnp.zeros(tot.shape, F32)
    acc[...] = jnp.zeros(acc.shape, F32)

    for k in range(1, chips):
        chip_copy(k).wait_recv()
        launch(k)

    slot_rows = CORES * chips * r

    def attend(slot, slots):
        start = slot * slot_rows
        if not isinstance(start, int):
            start = pl.multiple_of(start, slot_rows)
        for s in range(slots):
            for j in range(chips):
                mate_copy(slot + s, j).wait_recv()
        here = pl.ds(start, slots * slot_rows)
        scores = lax.dot_general(
            q2[...], kv[here, :head], (((1,), (1,)), ((), ())), preferred_element_type=F32
        ) * (head**-0.5)
        old = top[...]
        new = jnp.maximum(old, jnp.max(scores, axis=-1, keepdims=True))
        shrink = jnp.exp(old - new)
        probs = jnp.exp(scores - new)
        top[...] = new
        tot[...] = tot[...] * shrink + jnp.sum(probs, axis=-1, keepdims=True)
        acc[...] = acc[...] * shrink + jnp.dot(
            probs.astype(BF16), kv[here, head:], preferred_element_type=F32
        )

    def step(d, cw_on, cc_on):
        for j in range(chips):
            cw_copy(d, j).wait_recv()
            if j in cw_on:
                cw_copy(d + 1, j).start()
            mate_copy(cw_slot(d), j).start()
            cc_copy(d, j).wait_recv()
            if j in cc_on:
                cc_copy(d + 1, j).start()
            mate_copy(cc_slot(d), j).start()

    every = range(chips)
    few = range(0, last_cw) if last else range(0)
    others = range(last_cw, chips) if last else range(0)
    if full >= 1:
        step(1, every if full > 1 else few, every if full > 1 else others)
        attend(0, 1)
        if full > 6:

            def middle(d, carry):
                step(d, every, every)
                attend(2 * d - 3, 2)
                return carry

            lax.fori_loop(2, full, middle, 0)
        else:
            for d in range(2, full):
                step(d, every, every)
                attend(2 * d - 3, 2)
        if full > 1:
            step(full, few, others)
            attend(2 * full - 3, 2)
        tail_slot, tail_count = 2 * full - 1, 2
    else:
        tail_slot, tail_count = 0, 1
    if last:
        for j in every:
            (cw_copy if j < last_cw else cc_copy)(last, j).wait_recv()
            mate_copy(n - 1, j).start()
    attend(tail_slot, tail_count)
    if last:
        attend(n - 1, 1)

    attended = (acc[...] / tot[...]).astype(BF16)
    for h in range(heads_here):
        att[:, h * head : (h + 1) * head] = attended[h * tgt_rows : (h + 1) * tgt_rows, :]
    for copy in rest:
        copy.wait()

    def piece(c, side):
        return pl.ds(pl.multiple_of((c * CORES + side) * rs, rs), rs)

    def multiply_out(lhs, weight, send, recv, send_sem, recv_sem):
        for c in range(chunks):
            here = slice(c * cols, (c + 1) * cols)
            part[c] = jnp.dot(lhs, weight[:, here], preferred_element_type=F32)
            for k in range(chips):
                send[c, k * rs : (k + 1) * rs, :] = part[c, piece(k, 1 - core), :].astype(BF16)
            remote(send.at[c], recv.at[c], send_sem.at[c], recv_sem.at[c], (sp, mate)).start()

    def mate_wait(c, send, recv, send_sem, recv_sem):
        remote(send.at[c], recv.at[c], send_sem.at[c], recv_sem.at[c], (sp, mate)).wait_recv()

    multiply_out(att[...], ow, half_s, half_r, b_s, b_r)

    def wide_copy(k, c):
        return remote(
            chip_s.at[c],
            chip_r.at[k - 1, c],
            bx_s.at[k, c],
            bx_r.at[k, c],
            (sp, chip_at(k) * CORES + core),
        )

    for c in range(chunks):
        mate_wait(c, half_s, half_r, b_s, b_r)
        for k in range(chips):
            at = slice(k * rs, (k + 1) * rs)
            both = part[c, piece(k, core), :] + half_r[c, at, :].astype(F32)
            res[at, c * cols : (c + 1) * cols] = both
            chip_s[c, at, :] = both.astype(BF16)
        for k in range(1, chips):
            wide_copy(k, c).start()
    squares = jnp.zeros((half_rows, 1), F32)
    for c in range(chunks):
        here = slice(c * cols, (c + 1) * cols)
        projected = res[:, here]
        for k in range(1, chips):
            wide_copy(k, c).wait_recv()
            projected = projected + chip_r[k - 1, c].astype(F32)
        mine = jnp.concatenate([tgt[piece(k, core), here] for k in range(chips)], axis=0)
        residual = (mine.astype(F32) + projected).astype(BF16).astype(F32)
        res[:, here] = residual
        squares = squares + jnp.sum(residual * residual, axis=-1, keepdims=True)
    scale = lax.rsqrt(squares / width + EPS)

    def spot(k):
        return pl.ds(pl.multiple_of(HALO + (k * CORES + core) * rs, HALO), rs)

    def row_copy(k):
        return remote(
            rows_in.at[spot(k), :], rows_in.at[spot(k), :], m_s.at[k], m_r.at[k], (sp, mate)
        )

    def mate_row_copy(k):
        at = pl.ds(pl.multiple_of(HALO + (k * CORES + 1 - core) * rs, HALO), rs)
        return remote(rows_in.at[at, :], rows_in.at[at, :], m_s.at[k], m_r.at[k], (sp, mate))

    def halo_copy(i, t):
        return remote(
            rows_in.at[tgt_rows : tgt_rows + HALO, :],
            rows_in.at[0:HALO, :],
            h_s.at[i],
            h_r,
            (following, t),
        )

    sends_halo = jnp.logical_and(core == 1, sp < n - 1)
    for k in reversed(range(chips)):
        at = slice(k * rs, (k + 1) * rs)
        rows_in[spot(k), :] = (res[at, :] * scale[at, :] * mgain[...]).astype(BF16)
        if k == chips - 1:

            @pl.when(sends_halo)
            def _():
                halo_copy(0, mate).start()
                halo_copy(1, tp).start()

        row_copy(k).start()

    @pl.when(sp == 0)
    def _():
        rows_in[0:HALO, :] = jnp.zeros((HALO, width), BF16)

    for k in range(chips):
        mate_row_copy(k).wait_recv()

    @pl.when(sp > 0)
    def _():
        halo_copy(0, tp).wait_recv()

    hidden_cols = hid.shape[1]
    wide = conv_g.shape[1]
    taps = gtaps.shape[0]
    for f in range(hidden_cols // wide):
        here = slice(f * wide, (f + 1) * wide)
        all_rows = rows_in[...]
        conv_g[...] = jnp.dot(all_rows, gw[:, here], preferred_element_type=F32).astype(
            BF16
        ).astype(F32)
        conv_u[...] = jnp.dot(all_rows, uw[:, here], preferred_element_type=F32).astype(
            BF16
        ).astype(F32)
        gate = jnp.zeros((tgt_rows, wide), F32)
        up = jnp.zeros((tgt_rows, wide), F32)
        for t in range(taps):
            begin = HALO - (taps - 1) + t
            gate = gate + gtaps[t : t + 1, here].astype(F32) * conv_g[begin : begin + tgt_rows, :]
            up = up + utaps[t : t + 1, here].astype(F32) * conv_u[begin : begin + tgt_rows, :]
        hid[:, here] = (gate / (1.0 + jnp.exp(-gate)) * up).astype(BF16)

    multiply_out(hid[...], dw, tail_s, tail_r, f_s, f_r)

    def end_copy(k, c):
        there = chip_at(k)
        at = pl.ds(pl.multiple_of(there * rs, rs), rs)
        return remote(
            end_s.at[c, at, :],
            end_r.at[k - 1, c],
            fx_s.at[k, c],
            fx_r.at[k, c],
            (sp, there * CORES + core),
        )

    for c in range(chunks):
        mate_wait(c, tail_s, tail_r, f_s, f_r)
        for k in range(chips):
            at = slice(k * rs, (k + 1) * rs)
            both = part[c, piece(k, core), :] + tail_r[c, at, :].astype(F32)
            part[c, piece(k, core), :] = both
            end_s[c, at, :] = both.astype(BF16)
        for k in range(1, chips):
            end_copy(k, c).start()
    own = pl.ds(pl.multiple_of(chip * rs, rs), rs)
    squares = jnp.zeros((rs, 1), F32)
    sums = []
    for c in range(chunks):
        here = slice(c * cols, (c + 1) * cols)
        total = res[own, here] + part[c, piece(chip, core), :]
        for k in range(1, chips):
            end_copy(k, c).wait_recv()
            total = total + end_r[k - 1, c].astype(F32)
        squares = squares + jnp.sum(total * total, axis=-1, keepdims=True)
        sums.append(total)
    scale = lax.rsqrt(squares / width + EPS)
    for c in range(chunks):
        here = slice(c * cols, (c + 1) * cols)
        out_ref[:, here] = (sums[c] * scale * fgain[:, here]).astype(BF16)

    for k in range(1, chips):
        chip_copy(k).wait_send()
        for c in range(chunks):
            wide_copy(k, c).wait_send()
            end_copy(k, c).wait_send()
    for c in range(chunks):
        remote(half_s.at[c], half_r.at[c], b_s.at[c], b_r.at[c], (sp, mate)).wait_send()
        remote(tail_s.at[c], tail_r.at[c], f_s.at[c], f_r.at[c], (sp, mate)).wait_send()
    for k in range(chips):
        row_copy(k).wait_send()

    @pl.when(sends_halo)
    def _():
        halo_copy(0, mate).wait_send()
        halo_copy(1, tp).wait_send()

    def drain(d, carry):
        for j in every:
            cw_copy(d, j).wait_send()
            cc_copy(d, j).wait_send()
        return carry

    def drain_mate(slot, carry):
        for j in every:
            mate_copy(slot, j).wait_send()
        return carry

    if full >= 1:
        drain(1, 0)
    if full >= 2:
        lax.fori_loop(2, full + 1, drain, 0)
    if last:
        for j in every:
            (cw_copy if j < last_cw else cc_copy)(last, j).wait_send()
    lax.fori_loop(0, n, drain_mate, 0)


def solution(mesh):
    n = mesh.shape["sp"]
    chips = mesh.shape["tp"] // CORES
    head = 256

    def shards(*args):
        args = [a[None, :] if a.ndim == 1 else a for a in args]
        (target, source, _, _, qw, kw, _, ow, _, gw, _, _, _, dw, _) = args
        tgt_rows, width = target.shape
        r = source.shape[0]
        kv_heads = kw.shape[1] // head
        heads_here = qw.shape[1] // head
        rs = tgt_rows // (CORES * chips)
        half = chips * rs
        cols = 512
        chunks = width // cols
        ff = gw.shape[1]
        wide = 256 if ff % 256 == 0 else 128
        q_rows = heads_here * tgt_rows
        dists = n // 2 + 1
        dma = pltpu.SemaphoreType.DMA
        scratch = [pltpu.VMEM(a.shape, a.dtype) for a in args]
        scratch += [
            pltpu.VMEM((kv_heads, r, 2 * head), BF16),
            pltpu.VMEM((n * CORES * chips * r, 2 * head), BF16),
            pltpu.VMEM((q_rows, head), BF16),
            pltpu.VMEM((q_rows, 1), F32),
            pltpu.VMEM((q_rows, 1), F32),
            pltpu.VMEM((q_rows, head), F32),
            pltpu.VMEM((tgt_rows, heads_here * head), BF16),
            pltpu.VMEM((chunks, tgt_rows, cols), F32),
            pltpu.VMEM((chunks, half, cols), BF16),
            pltpu.VMEM((chunks, half, cols), BF16),
            pltpu.VMEM((chunks, half, cols), BF16),
            pltpu.VMEM((max(chips - 1, 1), chunks, half, cols), BF16),
            pltpu.VMEM((half, width), F32),
            pltpu.VMEM((HALO + tgt_rows, width), BF16),
            pltpu.VMEM((HALO + tgt_rows, wide), F32),
            pltpu.VMEM((HALO + tgt_rows, wide), F32),
            pltpu.VMEM((tgt_rows, ff), BF16),
            pltpu.VMEM((chunks, half, cols), BF16),
            pltpu.VMEM((chunks, half, cols), BF16),
            pltpu.VMEM((chunks, half, cols), BF16),
            pltpu.VMEM((max(chips - 1, 1), chunks, rs, cols), BF16),
            dma((len(args),)),
            dma((chips,)),
            dma((chips,)),
        ]
        scratch += [dma((dists, chips))] * 4
        scratch += [dma((n, chips))] * 2
        scratch += [dma((chunks,))] * 2
        scratch += [dma((chips, chunks))] * 2
        scratch += [dma((chips,))] * 2
        scratch += [dma((2,)), dma]
        scratch += [dma((chunks,))] * 2
        scratch += [dma((chips, chunks))] * 2
        return pl.pallas_call(
            functools.partial(layer, (n, chips, kv_heads, head, heads_here, cols)),
            out_shape=jax.ShapeDtypeStruct((rs, width), BF16),
            in_specs=[pl.BlockSpec(memory_space=pl.ANY)] * len(args),
            out_specs=pl.BlockSpec(memory_space=pltpu.VMEM),
            scratch_shapes=scratch,
            compiler_params=pltpu.CompilerParams(
                collective_id=0, has_side_effects=True, vmem_limit_bytes=60 * 1024 * 1024
            ),
        )(*args)

    in_specs = (
        P("sp", None),
        P(("sp", "tp"), None),
        P(),
        P(),
        P(None, "tp"),
        P(),
        P(),
        P("tp", None),
        P(),
        P(None, "tp"),
        P(None, "tp"),
        P(None, "tp"),
        P(None, "tp"),
        P("tp", None),
        P(),
    )
    return jax.shard_map(
        shards, mesh=mesh, in_specs=in_specs, out_specs=P(("sp", "tp"), None), check_vma=False
    )
```

```python
import functools

import jax
import jax.numpy as jnp
from jax import lax
from jax.experimental import pallas as pl
from jax.experimental.pallas import tpu as pltpu
from jax.sharding import PartitionSpec as P

MESH = pl.DeviceIdType.MESH
EPS = 1e-06
HALO = 16
RUN = 16
CORES = 2
F32 = jnp.float32
BF16 = jnp.bfloat16


def normed(values, gain):
    wide = values.astype(F32)
    scale = lax.rsqrt(jnp.mean(wide * wide, axis=-1, keepdims=True) + EPS)
    return (wide * scale * gain).astype(BF16)


def layer(
    dims,
    target_h,
    source_h,
    qgain_h,
    sgain_h,
    qw_h,
    kw_h,
    vw_h,
    ow_h,
    mgain_h,
    gw_h,
    uw_h,
    gtaps_h,
    utaps_h,
    dw_h,
    fgain_h,
    out_ref,
    tgt,
    src,
    qgain,
    sgain,
    qw,
    kw,
    vw,
    ow,
    mgain,
    gw,
    uw,
    gtaps,
    utaps,
    dw,
    fgain,
    kvh,
    kv,
    q2,
    top,
    tot,
    acc,
    att,
    part,
    half_s,
    half_r,
    chip_s,
    chip_r,
    res,
    rows_in,
    conv_g,
    conv_u,
    hid,
    tail_s,
    tail_r,
    end_s,
    end_r,
    load_sem,
    kx_s,
    kx_r,
    cw_s,
    cw_r,
    cc_s,
    cc_r,
    d2_s,
    d2_r,
    b_s,
    b_r,
    bx_s,
    bx_r,
    m_s,
    m_r,
    h_s,
    h_r,
    f_s,
    f_r,
    fx_s,
    fx_r,
):
    n, chips, kv_heads, head, heads_here, cols, sub = dims
    tgt_rows, width = tgt.shape
    r = src.shape[0]
    rs = tgt_rows // (CORES * chips)
    half_rows = chips * rs
    run = r // sub
    runs = chips * sub
    chunks = width // cols
    sp = lax.axis_index("sp")
    tp = lax.axis_index("tp")
    chip = tp // CORES
    core = tp % CORES
    mate = tp + 1 - 2 * core

    def chip_at(k):
        return (chip + k) % chips

    def ring_at(p):
        if n % 2:
            return p
        upper = p // (n // 2)
        return 2 * (p * (1 - upper) + (n - 1 - p) * upper) + upper

    if n % 2:
        pos = sp
    else:
        pos = (sp // 2) * (1 - sp % 2) + (n - 1 - sp // 2) * (sp % 2)
    ahead = ring_at((pos + 1) % n)
    behind = ring_at((pos + n - 1) % n)

    def load(index, hbm, vmem):
        copy = pltpu.make_async_copy(hbm, vmem, load_sem.at[index])
        copy.start()
        return copy

    def head_of(c):
        return (c * CORES * kv_heads) // (chips * CORES)

    own_head = head_of(chip)
    order = [(own_head + 1 + g) % kv_heads for g in range(kv_heads)]

    def columns(g):
        return pl.ds(pl.multiple_of(g * head, head), head)

    first = [load(0, source_h, src), load(1, sgain_h, sgain)]
    by_head = [
        [
            load(2 + 2 * i, kw_h.at[:, columns(g)], kw.at[:, columns(g)]),
            load(3 + 2 * i, vw_h.at[:, columns(g)], vw.at[:, columns(g)]),
        ]
        for i, g in enumerate(order)
    ]
    used = 2 + 2 * kv_heads

    barrier = pltpu.get_barrier_semaphore()
    following = (sp + 1) % n
    peers = [(ahead, tp), (behind, tp), (sp, mate)]
    peers += [(sp, chip_at(k) * CORES + core) for k in range(1, chips)]
    for peer in peers:
        pl.semaphore_signal(barrier, inc=1, device_id=peer, device_id_type=MESH)

    def remote(source_ref, dest_ref, send, recv, device):
        return pltpu.make_async_remote_copy(
            src_ref=source_ref,
            dst_ref=dest_ref,
            send_sem=send,
            recv_sem=recv,
            device_id=device,
            device_id_type=MESH,
        )

    def block(slot, lineage, j):
        start = ((slot * CORES + lineage) * runs + j) * run
        if not isinstance(start, int):
            start = pl.multiple_of(start, run)
        return kv.at[pl.ds(start, run), :]

    def chip_copy(j):
        there = chip_at(j // sub)
        return remote(
            kvh.at[head_of(there), (j % sub) * run : (j % sub + 1) * run, :],
            block(0, 0, j),
            kx_s.at[j],
            kx_r.at[j],
            (sp, there * CORES + core),
        )

    last = n // 2 if n % 2 == 0 else 0
    full = (n - 1) // 2
    if sub > 1:
        half_cw = [j for j in range(runs) if j % sub < sub // 2]
    else:
        half_cw = list(range((runs + 1) // 2))
    half_cc = [j for j in range(runs) if j not in half_cw]

    def cw_slot(d):
        return 2 * d - 1

    def cc_slot(d):
        return n - 1 if isinstance(d, int) and d == last else 2 * d

    def cw_copy(d, j):
        held = 0 if isinstance(d, int) and d == 1 else cw_slot(d - 1)
        return remote(
            block(held, 0, j), block(cw_slot(d), 0, j), cw_s.at[d, j], cw_r.at[d, j], (ahead, tp)
        )

    def cc_copy(d, j):
        held = 0 if isinstance(d, int) and d == 1 else 2 * (d - 1)
        return remote(
            block(held, 0, j), block(cc_slot(d), 0, j), cc_s.at[d, j], cc_r.at[d, j], (behind, tp)
        )

    def mate_copy(slot, j):
        return remote(
            block(slot, 0, j), block(slot, 1, j), d2_s.at[slot, j], d2_r.at[slot, j], (sp, mate)
        )

    def launch(j):
        if n > 2 or j in half_cw:
            cw_copy(1, j).start()
        if n > 2 or j in half_cc:
            cc_copy(1, j).start()
        mate_copy(0, j).start()

    for copy in first:
        copy.wait()
    source_in = normed(src[...], sgain[...])
    second = [
        load(used + i, a, b)
        for i, (a, b) in enumerate(((target_h, tgt), (qgain_h, qgain), (qw_h, qw)))
    ]
    early = chips == kv_heads
    for i, g in enumerate(order):
        for copy in by_head[i]:
            copy.wait()
        keys = jnp.dot(source_in, kw[:, columns(g)], preferred_element_type=F32)
        kvh[g, :, :head] = keys.astype(BF16)
        values = jnp.dot(source_in, vw[:, columns(g)], preferred_element_type=F32)
        kvh[g, :, head:] = values.astype(BF16)
        if i == (kv_heads - 2 if early else kv_heads - 1):
            pl.semaphore_wait(barrier, len(peers))
            for j in range(sub, runs):
                chip_copy(j).start()
    kv[0:r, :] = kvh[own_head]
    for j in range(sub):
        launch(j)
    rest = [
        load(used + 3 + i, a, b)
        for i, (a, b) in enumerate(
            (
                (ow_h, ow),
                (mgain_h, mgain),
                (gw_h, gw),
                (uw_h, uw),
                (gtaps_h, gtaps),
                (utaps_h, utaps),
                (dw_h, dw),
                (fgain_h, fgain),
            )
        )
    ]

    for copy in second:
        copy.wait()
    queries = jnp.dot(normed(tgt[...], qgain[...]), qw[...], preferred_element_type=F32).astype(
        BF16
    )
    for h in range(heads_here):
        q2[h * tgt_rows : (h + 1) * tgt_rows, :] = queries[:, h * head : (h + 1) * head]
    top[...] = jnp.full(top.shape, -1e30, F32)
    tot[...] = jnp.zeros(tot.shape, F32)
    acc[...] = jnp.zeros(acc.shape, F32)

    for j in range(sub, runs):
        chip_copy(j).wait_recv()
        launch(j)

    slot_rows = CORES * chips * r

    def attend(slot, slots):
        start = slot * slot_rows
        if not isinstance(start, int):
            start = pl.multiple_of(start, slot_rows)
        for s in range(slots):
            for j in range(runs):
                mate_copy(slot + s, j).wait_recv()
        here = pl.ds(start, slots * slot_rows)
        scores = lax.dot_general(
            q2[...], kv[here, :head], (((1,), (1,)), ((), ())), preferred_element_type=F32
        ) * (head**-0.5)
        old = top[...]
        new = jnp.maximum(old, jnp.max(scores, axis=-1, keepdims=True))
        shrink = jnp.exp(old - new)
        probs = jnp.exp(scores - new)
        top[...] = new
        tot[...] = tot[...] * shrink + jnp.sum(probs, axis=-1, keepdims=True)
        acc[...] = acc[...] * shrink + jnp.dot(
            probs.astype(BF16), kv[here, head:], preferred_element_type=F32
        )

    def step(d, cw_on, cc_on):
        for j in range(runs):
            cw_copy(d, j).wait_recv()
            if j in cw_on:
                cw_copy(d + 1, j).start()
            mate_copy(cw_slot(d), j).start()
            cc_copy(d, j).wait_recv()
            if j in cc_on:
                cc_copy(d + 1, j).start()
            mate_copy(cc_slot(d), j).start()

    every = range(runs)
    few = half_cw if last else []
    others = half_cc if last else []
    if full >= 1:
        step(1, every if full > 1 else few, every if full > 1 else others)
        attend(0, 1)
        if full > 6:

            def middle(d, carry):
                step(d, every, every)
                attend(2 * d - 3, 2)
                return carry

            lax.fori_loop(2, full, middle, 0)
        else:
            for d in range(2, full):
                step(d, every, every)
                attend(2 * d - 3, 2)
        if full > 1:
            step(full, few, others)
            attend(2 * full - 3, 2)
        tail_slot, tail_count = 2 * full - 1, 2
    else:
        tail_slot, tail_count = 0, 1
    if last:
        for j in every:
            (cw_copy if j in half_cw else cc_copy)(last, j).wait_recv()
            mate_copy(n - 1, j).start()
    attend(tail_slot, tail_count)
    if last:
        attend(n - 1, 1)

    attended = (acc[...] / tot[...]).astype(BF16)
    for h in range(heads_here):
        att[:, h * head : (h + 1) * head] = attended[h * tgt_rows : (h + 1) * tgt_rows, :]
    for copy in rest:
        copy.wait()

    def piece(c, side):
        return pl.ds(pl.multiple_of((c * CORES + side) * rs, rs), rs)

    def multiply_out(lhs, weight, send, recv, send_sem, recv_sem):
        for c in range(chunks):
            here = slice(c * cols, (c + 1) * cols)
            part[c] = jnp.dot(lhs, weight[:, here], preferred_element_type=F32)
            for k in range(chips):
                send[c, k * rs : (k + 1) * rs, :] = part[c, piece(k, 1 - core), :].astype(BF16)
            remote(send.at[c], recv.at[c], send_sem.at[c], recv_sem.at[c], (sp, mate)).start()

    def mate_wait(c, send, recv, send_sem, recv_sem):
        remote(send.at[c], recv.at[c], send_sem.at[c], recv_sem.at[c], (sp, mate)).wait_recv()

    multiply_out(att[...], ow, half_s, half_r, b_s, b_r)

    def wide_copy(k, c):
        return remote(
            chip_s.at[c],
            chip_r.at[k - 1, c],
            bx_s.at[k, c],
            bx_r.at[k, c],
            (sp, chip_at(k) * CORES + core),
        )

    for c in range(chunks):
        mate_wait(c, half_s, half_r, b_s, b_r)
        for k in range(chips):
            at = slice(k * rs, (k + 1) * rs)
            both = part[c, piece(k, core), :] + half_r[c, at, :].astype(F32)
            res[at, c * cols : (c + 1) * cols] = both
            chip_s[c, at, :] = both.astype(BF16)
        for k in range(1, chips):
            wide_copy(k, c).start()
    squares = jnp.zeros((half_rows, 1), F32)
    for c in range(chunks):
        here = slice(c * cols, (c + 1) * cols)
        projected = res[:, here]
        for k in range(1, chips):
            wide_copy(k, c).wait_recv()
            projected = projected + chip_r[k - 1, c].astype(F32)
        mine = jnp.concatenate([tgt[piece(k, core), here] for k in range(chips)], axis=0)
        residual = (mine.astype(F32) + projected).astype(BF16).astype(F32)
        res[:, here] = residual
        squares = squares + jnp.sum(residual * residual, axis=-1, keepdims=True)
    scale = lax.rsqrt(squares / width + EPS)

    def spot(k):
        return pl.ds(pl.multiple_of(HALO + (k * CORES + core) * rs, HALO), rs)

    def row_copy(k):
        return remote(
            rows_in.at[spot(k), :], rows_in.at[spot(k), :], m_s.at[k], m_r.at[k], (sp, mate)
        )

    def mate_row_copy(k):
        at = pl.ds(pl.multiple_of(HALO + (k * CORES + 1 - core) * rs, HALO), rs)
        return remote(rows_in.at[at, :], rows_in.at[at, :], m_s.at[k], m_r.at[k], (sp, mate))

    def halo_copy(i, t):
        return remote(
            rows_in.at[tgt_rows : tgt_rows + HALO, :],
            rows_in.at[0:HALO, :],
            h_s.at[i],
            h_r,
            (following, t),
        )

    sends_halo = jnp.logical_and(core == 1, sp < n - 1)
    for k in reversed(range(chips)):
        at = slice(k * rs, (k + 1) * rs)
        rows_in[spot(k), :] = (res[at, :] * scale[at, :] * mgain[...]).astype(BF16)
        if k == chips - 1:

            @pl.when(sends_halo)
            def _():
                halo_copy(0, mate).start()
                halo_copy(1, tp).start()

        row_copy(k).start()

    @pl.when(sp == 0)
    def _():
        rows_in[0:HALO, :] = jnp.zeros((HALO, width), BF16)

    for k in range(chips):
        mate_row_copy(k).wait_recv()

    @pl.when(sp > 0)
    def _():
        halo_copy(0, tp).wait_recv()

    hidden_cols = hid.shape[1]
    wide = conv_g.shape[1]
    taps = gtaps.shape[0]
    for f in range(hidden_cols // wide):
        here = slice(f * wide, (f + 1) * wide)
        all_rows = rows_in[...]
        conv_g[...] = jnp.dot(all_rows, gw[:, here], preferred_element_type=F32).astype(
            BF16
        ).astype(F32)
        conv_u[...] = jnp.dot(all_rows, uw[:, here], preferred_element_type=F32).astype(
            BF16
        ).astype(F32)
        gate = jnp.zeros((tgt_rows, wide), F32)
        up = jnp.zeros((tgt_rows, wide), F32)
        for t in range(taps):
            begin = HALO - (taps - 1) + t
            gate = gate + gtaps[t : t + 1, here].astype(F32) * conv_g[begin : begin + tgt_rows, :]
            up = up + utaps[t : t + 1, here].astype(F32) * conv_u[begin : begin + tgt_rows, :]
        hid[:, here] = (gate / (1.0 + jnp.exp(-gate)) * up).astype(BF16)

    multiply_out(hid[...], dw, tail_s, tail_r, f_s, f_r)

    def end_copy(k, c):
        there = chip_at(k)
        at = pl.ds(pl.multiple_of(there * rs, rs), rs)
        return remote(
            end_s.at[c, at, :],
            end_r.at[k - 1, c],
            fx_s.at[k, c],
            fx_r.at[k, c],
            (sp, there * CORES + core),
        )

    for c in range(chunks):
        mate_wait(c, tail_s, tail_r, f_s, f_r)
        for k in range(chips):
            at = slice(k * rs, (k + 1) * rs)
            both = part[c, piece(k, core), :] + tail_r[c, at, :].astype(F32)
            part[c, piece(k, core), :] = both
            end_s[c, at, :] = both.astype(BF16)
        for k in range(1, chips):
            end_copy(k, c).start()
    own = pl.ds(pl.multiple_of(chip * rs, rs), rs)
    squares = jnp.zeros((rs, 1), F32)
    sums = []
    for c in range(chunks):
        here = slice(c * cols, (c + 1) * cols)
        total = res[own, here] + part[c, piece(chip, core), :]
        for k in range(1, chips):
            end_copy(k, c).wait_recv()
            total = total + end_r[k - 1, c].astype(F32)
        squares = squares + jnp.sum(total * total, axis=-1, keepdims=True)
        sums.append(total)
    scale = lax.rsqrt(squares / width + EPS)
    for c in range(chunks):
        here = slice(c * cols, (c + 1) * cols)
        out_ref[:, here] = (sums[c] * scale * fgain[:, here]).astype(BF16)

    for j in range(sub, runs):
        chip_copy(j).wait_send()
    for k in range(1, chips):
        for c in range(chunks):
            wide_copy(k, c).wait_send()
            end_copy(k, c).wait_send()
    for c in range(chunks):
        remote(half_s.at[c], half_r.at[c], b_s.at[c], b_r.at[c], (sp, mate)).wait_send()
        remote(tail_s.at[c], tail_r.at[c], f_s.at[c], f_r.at[c], (sp, mate)).wait_send()
    for k in range(chips):
        row_copy(k).wait_send()

    @pl.when(sends_halo)
    def _():
        halo_copy(0, mate).wait_send()
        halo_copy(1, tp).wait_send()

    def drain(d, carry):
        for j in every:
            cw_copy(d, j).wait_send()
            cc_copy(d, j).wait_send()
        return carry

    def drain_mate(slot, carry):
        for j in every:
            mate_copy(slot, j).wait_send()
        return carry

    if full >= 1:
        drain(1, 0)
    if full >= 2:
        lax.fori_loop(2, full + 1, drain, 0)
    if last:
        for j in every:
            (cw_copy if j in half_cw else cc_copy)(last, j).wait_send()
    lax.fori_loop(0, n, drain_mate, 0)


def solution(mesh):
    n = mesh.shape["sp"]
    chips = mesh.shape["tp"] // CORES
    head = 256

    def shards(*args):
        args = [a[None, :] if a.ndim == 1 else a for a in args]
        (target, source, _, _, qw, kw, _, ow, _, gw, _, _, _, dw, _) = args
        tgt_rows, width = target.shape
        r = source.shape[0]
        kv_heads = kw.shape[1] // head
        heads_here = qw.shape[1] // head
        rs = tgt_rows // (CORES * chips)
        half = chips * rs
        cols = 512
        chunks = width // cols
        ff = gw.shape[1]
        wide = 256 if ff % 256 == 0 else 128
        q_rows = heads_here * tgt_rows
        dists = n // 2 + 1
        sub = max(r // RUN, 1)
        runs = chips * sub
        dma = pltpu.SemaphoreType.DMA
        scratch = [pltpu.VMEM(a.shape, a.dtype) for a in args]
        scratch += [
            pltpu.VMEM((kv_heads, r, 2 * head), BF16),
            pltpu.VMEM((n * CORES * chips * r, 2 * head), BF16),
            pltpu.VMEM((q_rows, head), BF16),
            pltpu.VMEM((q_rows, 1), F32),
            pltpu.VMEM((q_rows, 1), F32),
            pltpu.VMEM((q_rows, head), F32),
            pltpu.VMEM((tgt_rows, heads_here * head), BF16),
            pltpu.VMEM((chunks, tgt_rows, cols), F32),
            pltpu.VMEM((chunks, half, cols), BF16),
            pltpu.VMEM((chunks, half, cols), BF16),
            pltpu.VMEM((chunks, half, cols), BF16),
            pltpu.VMEM((max(chips - 1, 1), chunks, half, cols), BF16),
            pltpu.VMEM((half, width), F32),
            pltpu.VMEM((HALO + tgt_rows, width), BF16),
            pltpu.VMEM((HALO + tgt_rows, wide), F32),
            pltpu.VMEM((HALO + tgt_rows, wide), F32),
            pltpu.VMEM((tgt_rows, ff), BF16),
            pltpu.VMEM((chunks, half, cols), BF16),
            pltpu.VMEM((chunks, half, cols), BF16),
            pltpu.VMEM((chunks, half, cols), BF16),
            pltpu.VMEM((max(chips - 1, 1), chunks, rs, cols), BF16),
            dma((len(args) + 2 * kv_heads,)),
            dma((runs,)),
            dma((runs,)),
        ]
        scratch += [dma((dists, runs))] * 4
        scratch += [dma((n, runs))] * 2
        scratch += [dma((chunks,))] * 2
        scratch += [dma((chips, chunks))] * 2
        scratch += [dma((chips,))] * 2
        scratch += [dma((2,)), dma]
        scratch += [dma((chunks,))] * 2
        scratch += [dma((chips, chunks))] * 2
        return pl.pallas_call(
            functools.partial(layer, (n, chips, kv_heads, head, heads_here, cols, sub)),
            out_shape=jax.ShapeDtypeStruct((rs, width), BF16),
            in_specs=[pl.BlockSpec(memory_space=pl.ANY)] * len(args),
            out_specs=pl.BlockSpec(memory_space=pltpu.VMEM),
            scratch_shapes=scratch,
            compiler_params=pltpu.CompilerParams(
                collective_id=0, has_side_effects=True, vmem_limit_bytes=60 * 1024 * 1024
            ),
        )(*args)

    in_specs = (
        P("sp", None),
        P(("sp", "tp"), None),
        P(),
        P(),
        P(None, "tp"),
        P(),
        P(),
        P("tp", None),
        P(),
        P(None, "tp"),
        P(None, "tp"),
        P(None, "tp"),
        P(None, "tp"),
        P("tp", None),
        P(),
    )
    return jax.shard_map(
        shards, mesh=mesh, in_specs=in_specs, out_specs=P(("sp", "tp"), None), check_vma=False
    )
```

```python
import functools

import jax
import jax.numpy as jnp
from jax import lax
from jax.experimental import pallas as pl
from jax.experimental.pallas import tpu as pltpu
from jax.sharding import PartitionSpec as P

MESH = pl.DeviceIdType.MESH
EPS = 1e-06
HALO = 16
RUN = 32
CORES = 2
F32 = jnp.float32
BF16 = jnp.bfloat16


def normed(values, gain):
    wide = values.astype(F32)
    scale = lax.rsqrt(jnp.mean(wide * wide, axis=-1, keepdims=True) + EPS)
    return (wide * scale * gain).astype(BF16)


def layer(
    dims,
    target_h,
    source_h,
    qgain_h,
    sgain_h,
    qw_h,
    kw_h,
    vw_h,
    ow_h,
    mgain_h,
    gw_h,
    uw_h,
    gtaps_h,
    utaps_h,
    dw_h,
    fgain_h,
    out_ref,
    tgt,
    src,
    qgain,
    sgain,
    qw,
    kw,
    vw,
    ow,
    mgain,
    gw,
    uw,
    gtaps,
    utaps,
    dw,
    fgain,
    kvh,
    kv,
    q2,
    top,
    tot,
    acc,
    att,
    part,
    half_s,
    half_r,
    chip_s,
    chip_r,
    res,
    rows_in,
    conv_g,
    conv_u,
    hid,
    tail_s,
    tail_r,
    end_s,
    end_r,
    load_sem,
    kx_s,
    kx_r,
    cw_s,
    cw_r,
    cc_s,
    cc_r,
    d2_s,
    d2_r,
    b_s,
    b_r,
    bx_s,
    bx_r,
    m_s,
    m_r,
    h_s,
    h_r,
    f_s,
    f_r,
    fx_s,
    fx_r,
):
    n, chips, kv_heads, head, heads_here, cols, sub = dims
    tgt_rows, width = tgt.shape
    r = src.shape[0]
    rs = tgt_rows // (CORES * chips)
    half_rows = chips * rs
    run = r // sub
    runs = chips * sub
    chunks = width // cols
    sp = lax.axis_index("sp")
    tp = lax.axis_index("tp")
    chip = tp // CORES
    core = tp % CORES
    mate = tp + 1 - 2 * core

    def chip_at(k):
        return (chip + k) % chips

    def ring_at(p):
        if n % 2:
            return p
        upper = p // (n // 2)
        return 2 * (p * (1 - upper) + (n - 1 - p) * upper) + upper

    if n % 2:
        pos = sp
    else:
        pos = (sp // 2) * (1 - sp % 2) + (n - 1 - sp // 2) * (sp % 2)
    ahead = ring_at((pos + 1) % n)
    behind = ring_at((pos + n - 1) % n)

    def load(index, hbm, vmem):
        copy = pltpu.make_async_copy(hbm, vmem, load_sem.at[index])
        copy.start()
        return copy

    def head_of(c):
        return (c * CORES * kv_heads) // (chips * CORES)

    own_head = head_of(chip)
    order = [(own_head + 1 + g) % kv_heads for g in range(kv_heads)]

    def columns(g):
        return pl.ds(pl.multiple_of(g * head, head), head)

    first = [load(0, source_h, src), load(1, sgain_h, sgain)]
    by_head = [
        [
            load(2 + 2 * i, kw_h.at[:, columns(g)], kw.at[:, columns(g)]),
            load(3 + 2 * i, vw_h.at[:, columns(g)], vw.at[:, columns(g)]),
        ]
        for i, g in enumerate(order)
    ]
    used = 2 + 2 * kv_heads

    barrier = pltpu.get_barrier_semaphore()
    following = (sp + 1) % n
    peers = [(ahead, tp), (behind, tp), (sp, mate)]
    peers += [(sp, chip_at(k) * CORES + core) for k in range(1, chips)]
    for peer in peers:
        pl.semaphore_signal(barrier, inc=1, device_id=peer, device_id_type=MESH)

    def remote(source_ref, dest_ref, send, recv, device):
        return pltpu.make_async_remote_copy(
            src_ref=source_ref,
            dst_ref=dest_ref,
            send_sem=send,
            recv_sem=recv,
            device_id=device,
            device_id_type=MESH,
        )

    def block(slot, lineage, j):
        start = ((slot * CORES + lineage) * runs + j) * run
        if not isinstance(start, int):
            start = pl.multiple_of(start, run)
        return kv.at[pl.ds(start, run), :]

    def chip_copy(j):
        there = chip_at(j // sub)
        return remote(
            kvh.at[head_of(there), (j % sub) * run : (j % sub + 1) * run, :],
            block(0, 0, j),
            kx_s.at[j],
            kx_r.at[j],
            (sp, there * CORES + core),
        )

    last = n // 2 if n % 2 == 0 else 0
    full = (n - 1) // 2
    if sub > 1:
        half_cw = [j for j in range(runs) if j % sub < sub // 2]
    else:
        half_cw = list(range((runs + 1) // 2))
    half_cc = [j for j in range(runs) if j not in half_cw]

    def cw_slot(d):
        return 2 * d - 1

    def cc_slot(d):
        return n - 1 if isinstance(d, int) and d == last else 2 * d

    def cw_copy(d, j):
        held = 0 if isinstance(d, int) and d == 1 else cw_slot(d - 1)
        return remote(
            block(held, 0, j), block(cw_slot(d), 0, j), cw_s.at[d, j], cw_r.at[d, j], (ahead, tp)
        )

    def cc_copy(d, j):
        held = 0 if isinstance(d, int) and d == 1 else 2 * (d - 1)
        return remote(
            block(held, 0, j), block(cc_slot(d), 0, j), cc_s.at[d, j], cc_r.at[d, j], (behind, tp)
        )

    def mate_copy(slot, j):
        return remote(
            block(slot, 0, j), block(slot, 1, j), d2_s.at[slot, j], d2_r.at[slot, j], (sp, mate)
        )

    def launch(j):
        if n > 2 or j in half_cw:
            cw_copy(1, j).start()
        if n > 2 or j in half_cc:
            cc_copy(1, j).start()
        mate_copy(0, j).start()

    for copy in first:
        copy.wait()
    source_in = normed(src[...], sgain[...])
    second = [
        load(used + i, a, b)
        for i, (a, b) in enumerate(((target_h, tgt), (qgain_h, qgain), (qw_h, qw)))
    ]
    early = chips == kv_heads
    for i, g in enumerate(order):
        for copy in by_head[i]:
            copy.wait()
        keys = jnp.dot(source_in, kw[:, columns(g)], preferred_element_type=F32)
        kvh[g, :, :head] = keys.astype(BF16)
        values = jnp.dot(source_in, vw[:, columns(g)], preferred_element_type=F32)
        kvh[g, :, head:] = values.astype(BF16)
        if i == (kv_heads - 2 if early else kv_heads - 1):
            pl.semaphore_wait(barrier, len(peers))
            for j in range(sub, runs):
                chip_copy(j).start()
    kv[0:r, :] = kvh[own_head]
    for j in range(sub):
        launch(j)
    rest = [
        load(used + 3 + i, a, b)
        for i, (a, b) in enumerate(
            (
                (ow_h, ow),
                (mgain_h, mgain),
                (gw_h, gw),
                (uw_h, uw),
                (gtaps_h, gtaps),
                (utaps_h, utaps),
                (dw_h, dw),
                (fgain_h, fgain),
            )
        )
    ]

    for copy in second:
        copy.wait()
    queries = jnp.dot(normed(tgt[...], qgain[...]), qw[...], preferred_element_type=F32).astype(
        BF16
    )
    for h in range(heads_here):
        q2[h * tgt_rows : (h + 1) * tgt_rows, :] = queries[:, h * head : (h + 1) * head]
    top[...] = jnp.full(top.shape, -1e30, F32)
    tot[...] = jnp.zeros(tot.shape, F32)
    acc[...] = jnp.zeros(acc.shape, F32)

    for j in range(sub, runs):
        chip_copy(j).wait_recv()
        launch(j)

    slot_rows = CORES * chips * r

    def attend(slot, slots):
        start = slot * slot_rows
        if not isinstance(start, int):
            start = pl.multiple_of(start, slot_rows)
        for s in range(slots):
            for j in range(runs):
                mate_copy(slot + s, j).wait_recv()
        here = pl.ds(start, slots * slot_rows)
        scores = lax.dot_general(
            q2[...], kv[here, :head], (((1,), (1,)), ((), ())), preferred_element_type=F32
        ) * (head**-0.5)
        old = top[...]
        new = jnp.maximum(old, jnp.max(scores, axis=-1, keepdims=True))
        shrink = jnp.exp(old - new)
        probs = jnp.exp(scores - new)
        top[...] = new
        tot[...] = tot[...] * shrink + jnp.sum(probs, axis=-1, keepdims=True)
        acc[...] = acc[...] * shrink + jnp.dot(
            probs.astype(BF16), kv[here, head:], preferred_element_type=F32
        )

    def step(d, cw_on, cc_on):
        for j in range(runs):
            cw_copy(d, j).wait_recv()
            if j in cw_on:
                cw_copy(d + 1, j).start()
            mate_copy(cw_slot(d), j).start()
            cc_copy(d, j).wait_recv()
            if j in cc_on:
                cc_copy(d + 1, j).start()
            mate_copy(cc_slot(d), j).start()

    every = range(runs)
    few = half_cw if last else []
    others = half_cc if last else []
    if full >= 1:
        step(1, every if full > 1 else few, every if full > 1 else others)
        attend(0, 1)
        if full > 6:

            def middle(d, carry):
                step(d, every, every)
                attend(2 * d - 3, 2)
                return carry

            lax.fori_loop(2, full, middle, 0)
        else:
            for d in range(2, full):
                step(d, every, every)
                attend(2 * d - 3, 2)
        if full > 1:
            step(full, few, others)
            attend(2 * full - 3, 2)
        tail_slot, tail_count = 2 * full - 1, 2
    else:
        tail_slot, tail_count = 0, 1
    if last:
        for j in every:
            (cw_copy if j in half_cw else cc_copy)(last, j).wait_recv()
            mate_copy(n - 1, j).start()
    attend(tail_slot, tail_count)
    if last:
        attend(n - 1, 1)

    attended = (acc[...] / tot[...]).astype(BF16)
    for h in range(heads_here):
        att[:, h * head : (h + 1) * head] = attended[h * tgt_rows : (h + 1) * tgt_rows, :]
    for copy in rest:
        copy.wait()

    def piece(c, side):
        return pl.ds(pl.multiple_of((c * CORES + side) * rs, rs), rs)

    def multiply_out(lhs, weight, send, recv, send_sem, recv_sem):
        for c in range(chunks):
            here = slice(c * cols, (c + 1) * cols)
            part[c] = jnp.dot(lhs, weight[:, here], preferred_element_type=F32)
            for k in range(chips):
                send[c, k * rs : (k + 1) * rs, :] = part[c, piece(k, 1 - core), :].astype(BF16)
            remote(send.at[c], recv.at[c], send_sem.at[c], recv_sem.at[c], (sp, mate)).start()

    def mate_wait(c, send, recv, send_sem, recv_sem):
        remote(send.at[c], recv.at[c], send_sem.at[c], recv_sem.at[c], (sp, mate)).wait_recv()

    multiply_out(att[...], ow, half_s, half_r, b_s, b_r)

    def wide_copy(k, c):
        return remote(
            chip_s.at[c],
            chip_r.at[k - 1, c],
            bx_s.at[k, c],
            bx_r.at[k, c],
            (sp, chip_at(k) * CORES + core),
        )

    for c in range(chunks):
        mate_wait(c, half_s, half_r, b_s, b_r)
        for k in range(chips):
            at = slice(k * rs, (k + 1) * rs)
            both = part[c, piece(k, core), :] + half_r[c, at, :].astype(F32)
            res[at, c * cols : (c + 1) * cols] = both
            chip_s[c, at, :] = both.astype(BF16)
        for k in range(1, chips):
            wide_copy(k, c).start()
    squares = jnp.zeros((half_rows, 1), F32)
    for c in range(chunks):
        here = slice(c * cols, (c + 1) * cols)
        projected = res[:, here]
        for k in range(1, chips):
            wide_copy(k, c).wait_recv()
            projected = projected + chip_r[k - 1, c].astype(F32)
        mine = jnp.concatenate([tgt[piece(k, core), here] for k in range(chips)], axis=0)
        residual = (mine.astype(F32) + projected).astype(BF16).astype(F32)
        res[:, here] = residual
        squares = squares + jnp.sum(residual * residual, axis=-1, keepdims=True)
    scale = lax.rsqrt(squares / width + EPS)

    def spot(k):
        return pl.ds(pl.multiple_of(HALO + (k * CORES + core) * rs, HALO), rs)

    def row_copy(k):
        return remote(
            rows_in.at[spot(k), :], rows_in.at[spot(k), :], m_s.at[k], m_r.at[k], (sp, mate)
        )

    def mate_row_copy(k):
        at = pl.ds(pl.multiple_of(HALO + (k * CORES + 1 - core) * rs, HALO), rs)
        return remote(rows_in.at[at, :], rows_in.at[at, :], m_s.at[k], m_r.at[k], (sp, mate))

    def halo_copy(i, t):
        return remote(
            rows_in.at[tgt_rows : tgt_rows + HALO, :],
            rows_in.at[0:HALO, :],
            h_s.at[i],
            h_r,
            (following, t),
        )

    sends_halo = jnp.logical_and(core == 1, sp < n - 1)
    for k in reversed(range(chips)):
        at = slice(k * rs, (k + 1) * rs)
        rows_in[spot(k), :] = (res[at, :] * scale[at, :] * mgain[...]).astype(BF16)
        if k == chips - 1:

            @pl.when(sends_halo)
            def _():
                halo_copy(0, mate).start()
                halo_copy(1, tp).start()

        row_copy(k).start()

    @pl.when(sp == 0)
    def _():
        rows_in[0:HALO, :] = jnp.zeros((HALO, width), BF16)

    for k in range(chips):
        mate_row_copy(k).wait_recv()

    @pl.when(sp > 0)
    def _():
        halo_copy(0, tp).wait_recv()

    hidden_cols = hid.shape[1]
    wide = conv_g.shape[1]
    taps = gtaps.shape[0]
    for f in range(hidden_cols // wide):
        here = slice(f * wide, (f + 1) * wide)
        all_rows = rows_in[...]
        conv_g[...] = jnp.dot(all_rows, gw[:, here], preferred_element_type=F32).astype(
            BF16
        ).astype(F32)
        conv_u[...] = jnp.dot(all_rows, uw[:, here], preferred_element_type=F32).astype(
            BF16
        ).astype(F32)
        gate = jnp.zeros((tgt_rows, wide), F32)
        up = jnp.zeros((tgt_rows, wide), F32)
        for t in range(taps):
            begin = HALO - (taps - 1) + t
            gate = gate + gtaps[t : t + 1, here].astype(F32) * conv_g[begin : begin + tgt_rows, :]
            up = up + utaps[t : t + 1, here].astype(F32) * conv_u[begin : begin + tgt_rows, :]
        hid[:, here] = (gate / (1.0 + jnp.exp(-gate)) * up).astype(BF16)

    multiply_out(hid[...], dw, tail_s, tail_r, f_s, f_r)

    def end_copy(k, c):
        there = chip_at(k)
        at = pl.ds(pl.multiple_of(there * rs, rs), rs)
        return remote(
            end_s.at[c, at, :],
            end_r.at[k - 1, c],
            fx_s.at[k, c],
            fx_r.at[k, c],
            (sp, there * CORES + core),
        )

    for c in range(chunks):
        mate_wait(c, tail_s, tail_r, f_s, f_r)
        for k in range(chips):
            at = slice(k * rs, (k + 1) * rs)
            both = part[c, piece(k, core), :] + tail_r[c, at, :].astype(F32)
            part[c, piece(k, core), :] = both
            end_s[c, at, :] = both.astype(BF16)
        for k in range(1, chips):
            end_copy(k, c).start()
    own = pl.ds(pl.multiple_of(chip * rs, rs), rs)
    squares = jnp.zeros((rs, 1), F32)
    sums = []
    for c in range(chunks):
        here = slice(c * cols, (c + 1) * cols)
        total = res[own, here] + part[c, piece(chip, core), :]
        for k in range(1, chips):
            end_copy(k, c).wait_recv()
            total = total + end_r[k - 1, c].astype(F32)
        squares = squares + jnp.sum(total * total, axis=-1, keepdims=True)
        sums.append(total)
    scale = lax.rsqrt(squares / width + EPS)
    for c in range(chunks):
        here = slice(c * cols, (c + 1) * cols)
        out_ref[:, here] = (sums[c] * scale * fgain[:, here]).astype(BF16)

    for j in range(sub, runs):
        chip_copy(j).wait_send()
    for k in range(1, chips):
        for c in range(chunks):
            wide_copy(k, c).wait_send()
            end_copy(k, c).wait_send()
    for c in range(chunks):
        remote(half_s.at[c], half_r.at[c], b_s.at[c], b_r.at[c], (sp, mate)).wait_send()
        remote(tail_s.at[c], tail_r.at[c], f_s.at[c], f_r.at[c], (sp, mate)).wait_send()
    for k in range(chips):
        row_copy(k).wait_send()

    @pl.when(sends_halo)
    def _():
        halo_copy(0, mate).wait_send()
        halo_copy(1, tp).wait_send()

    def drain(d, carry):
        for j in every:
            cw_copy(d, j).wait_send()
            cc_copy(d, j).wait_send()
        return carry

    def drain_mate(slot, carry):
        for j in every:
            mate_copy(slot, j).wait_send()
        return carry

    if full >= 1:
        drain(1, 0)
    if full >= 2:
        lax.fori_loop(2, full + 1, drain, 0)
    if last:
        for j in every:
            (cw_copy if j in half_cw else cc_copy)(last, j).wait_send()
    lax.fori_loop(0, n, drain_mate, 0)


def solution(mesh):
    n = mesh.shape["sp"]
    chips = mesh.shape["tp"] // CORES
    head = 256

    def shards(*args):
        args = [a[None, :] if a.ndim == 1 else a for a in args]
        (target, source, _, _, qw, kw, _, ow, _, gw, _, _, _, dw, _) = args
        tgt_rows, width = target.shape
        r = source.shape[0]
        kv_heads = kw.shape[1] // head
        heads_here = qw.shape[1] // head
        rs = tgt_rows // (CORES * chips)
        half = chips * rs
        cols = width // 2
        chunks = width // cols
        ff = gw.shape[1]
        wide = 256 if ff % 256 == 0 else 128
        q_rows = heads_here * tgt_rows
        dists = n // 2 + 1
        sub = max(r // RUN, 1)
        runs = chips * sub
        dma = pltpu.SemaphoreType.DMA
        scratch = [pltpu.VMEM(a.shape, a.dtype) for a in args]
        scratch += [
            pltpu.VMEM((kv_heads, r, 2 * head), BF16),
            pltpu.VMEM((n * CORES * chips * r, 2 * head), BF16),
            pltpu.VMEM((q_rows, head), BF16),
            pltpu.VMEM((q_rows, 1), F32),
            pltpu.VMEM((q_rows, 1), F32),
            pltpu.VMEM((q_rows, head), F32),
            pltpu.VMEM((tgt_rows, heads_here * head), BF16),
            pltpu.VMEM((chunks, tgt_rows, cols), F32),
            pltpu.VMEM((chunks, half, cols), BF16),
            pltpu.VMEM((chunks, half, cols), BF16),
            pltpu.VMEM((chunks, half, cols), BF16),
            pltpu.VMEM((max(chips - 1, 1), chunks, half, cols), BF16),
            pltpu.VMEM((half, width), F32),
            pltpu.VMEM((HALO + tgt_rows, width), BF16),
            pltpu.VMEM((HALO + tgt_rows, wide), F32),
            pltpu.VMEM((HALO + tgt_rows, wide), F32),
            pltpu.VMEM((tgt_rows, ff), BF16),
            pltpu.VMEM((chunks, half, cols), BF16),
            pltpu.VMEM((chunks, half, cols), BF16),
            pltpu.VMEM((chunks, half, cols), BF16),
            pltpu.VMEM((max(chips - 1, 1), chunks, rs, cols), BF16),
            dma((len(args) + 2 * kv_heads,)),
            dma((runs,)),
            dma((runs,)),
        ]
        scratch += [dma((dists, runs))] * 4
        scratch += [dma((n, runs))] * 2
        scratch += [dma((chunks,))] * 2
        scratch += [dma((chips, chunks))] * 2
        scratch += [dma((chips,))] * 2
        scratch += [dma((2,)), dma]
        scratch += [dma((chunks,))] * 2
        scratch += [dma((chips, chunks))] * 2
        return pl.pallas_call(
            functools.partial(layer, (n, chips, kv_heads, head, heads_here, cols, sub)),
            out_shape=pltpu.VMEM((rs, width), BF16),
            in_specs=[pl.BlockSpec(memory_space=pl.ANY)] * len(args),
            out_specs=pl.BlockSpec(memory_space=pltpu.VMEM),
            scratch_shapes=scratch,
            compiler_params=pltpu.CompilerParams(
                collective_id=0, has_side_effects=True, vmem_limit_bytes=60 * 1024 * 1024
            ),
        )(*args)

    in_specs = (
        P("sp", None),
        P(("sp", "tp"), None),
        P(),
        P(),
        P(None, "tp"),
        P(),
        P(),
        P("tp", None),
        P(),
        P(None, "tp"),
        P(None, "tp"),
        P(None, "tp"),
        P(None, "tp"),
        P("tp", None),
        P(),
    )
    return jax.shard_map(
        shards, mesh=mesh, in_specs=in_specs, out_specs=P(("sp", "tp"), None), check_vma=False
    )
```
